32 devices in a mesh: grp: 2 (over y), kv: 4 (over z), tp: 4 (over x, core).
Axes of the slice: x: 2, y: 2, z: 4, core: 2. Of those that a mesh axis runs over, the one named last changes fastest.
Arguments:
- piece_tokens: bfloat16 [2048, 2048], P(('grp', 'kv')), parts along dimension 0, may hold values from -6 to 6
- dec_tokens: bfloat16 [32, 2048], P(('grp', 'kv')), parts along dimension 0, may hold values from -6 to 6
- norm_gain: float32 [2048], replicated, may hold values from 0.1 to 1.9
- query_weight: bfloat16 [2048, 1024], P(None, 'tp'), may hold values from -0.125 to 0.125
- key_weight: bfloat16 [2048, 1024], P(None, 'tp'), may hold values from -0.125 to 0.125
- value_weight: bfloat16 [2048, 1024], P(None, 'tp'), may hold values from -0.125 to 0.125
- forget_weight: bfloat16 [2048, 8], P(None, 'tp'), may hold values from -0.125 to 0.125
- forget_bias: float32 [8], P('tp'), may hold values from 3 to 13
- out_weight: bfloat16 [1024, 2048], P(None, 'tp'), may hold values from -0.1875 to 0.1875
- cache_keys: bfloat16 [32768, 1024], P(('grp', 'kv'), 'tp'), parts along dimension 0, may hold values from -480 to 480
- cache_values: bfloat16 [32768, 1024], P(('grp', 'kv'), 'tp'), parts along dimension 0, may hold values from -6 to 6
- cache_gates: float32 [8, 32768], P('tp', ('grp', 'kv')), parts along dimension 1, as said below
- dec_keys: bfloat16 [32, 2048, 1024], P(('grp', 'kv'), None, 'tp'), parts along dimension 0, may hold values from -480 to 480
- dec_values: bfloat16 [32, 2048, 1024], P(('grp', 'kv'), None, 'tp'), parts along dimension 0, may hold values from -6 to 6
- dec_gates: float32 [32, 8, 2048], P(('grp', 'kv'), 'tp'), parts along dimension 0, as said below
- dec_lengths: int32 [32], P(('grp', 'kv')), parts along dimension 0, may hold values from 1 to 2048, as said below
Outputs:
- piece_out: bfloat16 [2048, 2048], P(('grp', 'kv'), 'tp'), parts along dimension 0
- dec_out: bfloat16 [32, 2048], P(('grp', 'kv'), 'tp'), parts along dimension 0
- piece_keys: bfloat16 [2048, 1024], P(('grp', 'kv'), 'tp'), parts along dimension 0
- piece_values: bfloat16 [2048, 1024], P(('grp', 'kv'), 'tp'), parts along dimension 0
The draws below stay inside these ranges and needn't reach their ends.
There are 2 independent parts, one for each index of `grp`. The reference program is written for one: setup_inputs(seed, part) draws one part's arguments, and reference() takes and returns one part's arrays. A program takes and returns all parts, laid end to end along the dimension named above; an argument that names none is the same for every part. Nothing has to cross between parts.
Inputs may be any that keep to these rules, and one draw needn't show every extreme that they name: cache_gates never falls along positions and is 0 at the last cached position. dec_gates never falls along a sequence's live slots and is 0 at its last live slot and beyond. Slots 0 to dec_lengths[b] - 1 of sequence b are live; some sequence has exactly 2048.
All inputs are finite; a program needn't handle non-finite values.
Results may differ from the reference program's by a relative error of at most 0.015.
Values may be sent and summed in bfloat16 or wider, within the bound.
A program may use at most 128 MiB of HBM per device.

```python
import math
import jax
import jax.numpy as jnp
from jax import lax

D = 2048
HEADS = 8
HEAD_DIM = 128
PIECE_DEV = 256
CACHE_DEV = 4096
DLEN = 2048
WIDTH = 1024
PIECE = 1024
CACHE = 16384
DEC = 16
N_KV = 4


def head_slowness(key):
    order = jax.random.permutation(jax.random.fold_in(key, 3), HEADS)
    slow_heads = order < HEADS // 2
    return slow_heads


def live_lengths(key):
    base_length = jax.random.randint(jax.random.fold_in(key, 21), (DEC,), 1, DLEN + 1)
    shifts = jax.random.randint(jax.random.fold_in(key, 22), (DEC,), 0, 3)
    lengths = jnp.maximum(jnp.right_shift(base_length, shifts), 1)
    chosen = jax.random.randint(jax.random.fold_in(key, 23), (), 0, DEC)
    return jnp.where(jnp.arange(DEC) == chosen, DLEN, lengths).astype(jnp.int32)


def draw_forget_bias(key, part):
    slow_heads = head_slowness(key)
    slow_level = max(math.log(0.5 * PIECE), math.log(200.0))
    levels = jnp.where(slow_heads, slow_level, jnp.log(50.0))
    jitter = jax.random.uniform(jax.random.fold_in(key, 4), (HEADS,), jnp.float32, -0.3, 0.3)
    return (levels + jitter).astype(jnp.float32)


def draw_cache_gates(key, part):
    slow_heads = head_slowness(jax.random.fold_in(key, 5))
    levels = jnp.where(slow_heads, jnp.log(1.6 * (CACHE + PIECE)), jnp.log(50.0))
    noise = jax.random.normal(jax.random.fold_in(key, 6), (HEADS, CACHE), jnp.float32) * 0.7
    span_count = CACHE // CACHE_DEV
    factors = jnp.exp(jax.random.uniform(jax.random.fold_in(key, 7), (HEADS, span_count), jnp.float32, -0.7, 0.7))
    factors = jnp.repeat(factors, CACHE_DEV, axis=1)
    rates = jnp.exp(-levels[:, None] - noise) * factors
    suffix = jnp.cumsum(rates[:, ::-1], axis=1)[:, ::-1] - rates
    return (-suffix).astype(jnp.float32)


def draw_dec_gates(key, part):
    slow_heads = head_slowness(jax.random.fold_in(key, 8))
    levels = jnp.where(slow_heads, jnp.log(1.6 * DLEN), jnp.log(50.0))
    noise = jax.random.normal(jax.random.fold_in(key, 9), (DEC, HEADS, DLEN), jnp.float32) * 0.7
    factors = jnp.exp(jax.random.uniform(jax.random.fold_in(key, 10), (DEC, HEADS, 1), jnp.float32, -0.7, 0.7))
    lengths = live_lengths(key)
    live_slots = jnp.arange(DLEN)[None, None, :] < lengths[:, None, None]
    rates = jnp.where(live_slots, jnp.exp(-levels[None, :, None] - noise) * factors, 0.0)
    suffix = jnp.cumsum(rates[:, :, ::-1], axis=2)[:, :, ::-1] - rates
    return (-suffix).astype(jnp.float32)


def draw_dec_lengths(key, part):
    return live_lengths(key)


def draw_cache_keys(key, part):
    values = jnp.clip(jax.random.normal(jax.random.fold_in(key, 11), (CACHE, WIDTH), jnp.float32), -6.0, 6.0)
    return values.astype(jnp.bfloat16)


def draw_dec_keys(key, part):
    values = jnp.clip(jax.random.normal(jax.random.fold_in(key, 13), (DEC, DLEN, WIDTH), jnp.float32), -6.0, 6.0)
    return values.astype(jnp.bfloat16)


def steps_of(own_key, shape, shards, least, largest):
    loudness, own = 1.0, jax.random.fold_in(own_key, 6)
    for position, blocks in shards:
        heights = jnp.exp(jax.random.uniform(jax.random.fold_in(own, position), (blocks,), jnp.float32, least / len(shards), largest / len(shards)))
        loudness = loudness * jnp.repeat(heights, shape[position] // blocks).reshape([-1 if axis == position else 1 for axis in range(len(shape))])
    return loudness


def scatter_about(rng, dims, width, bound, shards=(), held_as=jnp.bfloat16):
    values = width * jax.random.normal(rng, dims, jnp.float32)
    if shards:
        values = values * steps_of(rng, dims, shards, -0.22, 0.18)
    return jnp.clip(values, -bound, bound).astype(held_as)


def setup_inputs(seed: int = 0, part: int = 0) -> dict:
    key_list = jax.random.split(jax.random.key(seed), 17)
    part_keys = jax.random.split(jax.random.fold_in(key_list[16], part), 17)
    return {
        "piece_tokens": scatter_about(part_keys[0], (PIECE, D), 1.0, 6.0, ((0, 4),)),
        "dec_tokens": scatter_about(part_keys[1], (DEC, D), 1.0, 6.0, ((0, 4),)),
        "norm_gain": jnp.clip(1.0 + 0.18 * jax.random.normal(key_list[2], (D,), jnp.float32), 0.1, 1.9),
        "query_weight": scatter_about(key_list[3], (D, WIDTH), D ** -0.5, 0.125, ((1, 4),)),
        "key_weight": scatter_about(key_list[4], (D, WIDTH), D ** -0.5, 0.125, ((1, 4),)),
        "value_weight": scatter_about(key_list[5], (D, WIDTH), D ** -0.5, 0.125, ((1, 4),)),
        "forget_weight": scatter_about(key_list[6], (D, HEADS), D ** -0.5, 0.125, ((1, 4),)),
        "forget_bias": draw_forget_bias(jax.random.fold_in(key_list[16], 71), part),
        "out_weight": scatter_about(key_list[8], (WIDTH, D), WIDTH ** -0.5, 0.1875, ((1, 4),)),
        "cache_keys": draw_cache_keys(jax.random.fold_in(jax.random.fold_in(key_list[16], part), 71), part),
        "cache_values": scatter_about(part_keys[10], (CACHE, WIDTH), 1.0, 6.0, ((0, 4), (1, 4))),
        "cache_gates": draw_cache_gates(jax.random.fold_in(jax.random.fold_in(key_list[16], part), 71), part),
        "dec_keys": draw_dec_keys(jax.random.fold_in(jax.random.fold_in(key_list[16], part), 71), part),
        "dec_values": scatter_about(part_keys[13], (DEC, DLEN, WIDTH), 1.0, 6.0, ((0, 4), (2, 4))),
        "dec_gates": draw_dec_gates(jax.random.fold_in(jax.random.fold_in(key_list[16], part), 71), part),
        "dec_lengths": draw_dec_lengths(jax.random.fold_in(jax.random.fold_in(key_list[16], part), 71), part),
    }


norm_eps = 1e-05

def rms_norm(tokens, norm_gain):
    values = tokens.astype(jnp.float32)
    factor = lax.rsqrt(lax.optimization_barrier(jnp.mean(values * values, axis=-1, keepdims=True)) + norm_eps)
    return (values * factor * norm_gain.astype(jnp.float32)).astype(jnp.bfloat16)

def project(tokens, norm_gain, query_weight, key_weight, value_weight, forget_weight, forget_bias):
    normed = rms_norm(tokens, norm_gain)
    queries = jnp.dot(normed, query_weight, preferred_element_type=jnp.float32).astype(jnp.bfloat16)
    key_rows = jnp.dot(normed, key_weight, preferred_element_type=jnp.float32).astype(jnp.bfloat16)
    value_rows = jnp.dot(normed, value_weight, preferred_element_type=jnp.float32).astype(jnp.bfloat16)
    log_gates = jax.nn.log_sigmoid(jnp.dot(normed, forget_weight, preferred_element_type=jnp.float32) + forget_bias.astype(jnp.float32))
    return (queries, key_rows, value_rows, log_gates)

def reference(piece_tokens, dec_tokens, norm_gain, query_weight, key_weight, value_weight, forget_weight, forget_bias, out_weight, cache_keys, cache_values, cache_gates, dec_keys, dec_values, dec_gates, dec_lengths):
    piece_queries, piece_keys, piece_values, piece_gates = project(piece_tokens, norm_gain, query_weight, key_weight, value_weight, forget_weight, forget_bias)
    dec_queries, dec_new_keys, dec_new_values, dec_gate_now = project(dec_tokens, norm_gain, query_weight, key_weight, value_weight, forget_weight, forget_bias)
    score_scale = HEAD_DIM ** (-0.5)
    prefix = jnp.cumsum(piece_gates, axis=0)
    piece_bias = -prefix.T
    block_rows = math.gcd(PIECE, 1024)
    block_count = PIECE // block_rows
    query_blocks = piece_queries.astype(jnp.float32).reshape(block_count, block_rows, HEADS, HEAD_DIM)
    block_starts = jnp.arange(block_count, dtype=jnp.int32) * block_rows

    def shard_keys(shard_number):
        cache_first = (shard_number * CACHE_DEV).astype(jnp.int32)
        piece_first = (shard_number * PIECE_DEV).astype(jnp.int32)
        key_rows = jnp.concatenate([lax.dynamic_slice_in_dim(cache_keys, cache_first, CACHE_DEV, 0), lax.dynamic_slice_in_dim(piece_keys, piece_first, PIECE_DEV, 0)], 0)
        value_rows = jnp.concatenate([lax.dynamic_slice_in_dim(cache_values, cache_first, CACHE_DEV, 0), lax.dynamic_slice_in_dim(piece_values, piece_first, PIECE_DEV, 0)], 0)
        key_bias = jnp.concatenate([lax.dynamic_slice_in_dim(cache_gates, cache_first, CACHE_DEV, 1), lax.dynamic_slice_in_dim(piece_bias, piece_first, PIECE_DEV, 1)], 1)
        key_order = jnp.concatenate([jnp.full((CACHE_DEV,), -1, jnp.int32), piece_first + jnp.arange(PIECE_DEV, dtype=jnp.int32)])
        key_rows = key_rows.astype(jnp.float32).reshape(-1, HEADS, HEAD_DIM)
        value_rows = value_rows.astype(jnp.float32).reshape(-1, HEADS, HEAD_DIM)
        return (key_rows, value_rows, key_bias, key_order)

    def block_scores(key_rows, key_bias, key_order, query_block, first_row):
        scores = jnp.einsum('qhd,khd->hqk', query_block, key_rows) * score_scale + key_bias[:, None, :]
        query_order = first_row + jnp.arange(block_rows, dtype=jnp.int32)
        visible = key_order[None, :] <= query_order[:, None]
        return jnp.where(visible[None], scores, -jnp.inf)

    def shard_terms(shard_number):
        key_rows, value_rows, key_bias, key_order = shard_keys(shard_number)

        def one_block(inputs):
            query_block, first_row = inputs
            scores = block_scores(key_rows, key_bias, key_order, query_block, first_row)
            local_max = lax.optimization_barrier(jnp.max(scores, axis=-1))
            weights_exp = jnp.exp(scores - local_max[:, :, None])
            rounded = lax.optimization_barrier(weights_exp.astype(jnp.bfloat16)).astype(jnp.float32)
            numerator = jnp.einsum('hqk,khd->qhd', rounded, value_rows).astype(jnp.bfloat16)
            return (numerator, lax.optimization_barrier(jnp.sum(weights_exp, axis=-1)), local_max)
        return lax.map(one_block, (query_blocks, block_starts))
    shard_numbers = jnp.arange(N_KV, dtype=jnp.int32)
    numerators, denominators, local_maxima = lax.map(shard_terms, shard_numbers)
    maxima = lax.optimization_barrier(jnp.max(local_maxima, axis=0))
    factors = jnp.exp(local_maxima - maxima[None])
    factor_rows = jnp.transpose(factors, (0, 1, 3, 2))[..., None]
    scaled = (numerators.astype(jnp.float32) * factor_rows).astype(jnp.bfloat16)
    scaled = lax.optimization_barrier(scaled).astype(jnp.float32)
    numer_sum = lax.optimization_barrier(jnp.sum(scaled, axis=0))
    denom_sum = jnp.transpose(lax.optimization_barrier(jnp.sum(denominators * factors, axis=0)), (0, 2, 1))
    piece_attention = (numer_sum / denom_sum[..., None]).astype(jnp.bfloat16).reshape(PIECE, HEADS * HEAD_DIM)

    def one_sequence(inputs):
        query_row, new_key, new_value, gate_now, seq_keys, seq_values, seq_gates, seq_length = inputs
        query_heads = query_row.astype(jnp.float32).reshape(HEADS, HEAD_DIM)
        key_heads = seq_keys.astype(jnp.float32).reshape(DLEN, HEADS, HEAD_DIM)
        value_heads = seq_values.astype(jnp.float32).reshape(DLEN, HEADS, HEAD_DIM)
        cached = jnp.einsum('hd,khd->hk', query_heads, key_heads) * score_scale + seq_gates + gate_now[:, None]
        live_slots = jnp.arange(DLEN, dtype=jnp.int32) < seq_length
        cached = jnp.where(live_slots[None, :], cached, -jnp.inf)
        own_score = lax.optimization_barrier(jnp.sum(query_heads * new_key.astype(jnp.float32).reshape(HEADS, HEAD_DIM), axis=-1)) * score_scale
        row_top = jnp.maximum(lax.optimization_barrier(jnp.max(cached, axis=-1)), own_score)
        cached_exp = jnp.exp(cached - row_top[:, None])
        own_exp = jnp.exp(own_score - row_top)
        whole_sum = lax.optimization_barrier(jnp.sum(cached_exp, axis=-1)) + own_exp
        cached_weights = (cached_exp / whole_sum[:, None]).astype(jnp.bfloat16).astype(jnp.float32)
        own_weights = (own_exp / whole_sum).astype(jnp.bfloat16).astype(jnp.float32)
        mixed = jnp.einsum('hk,khd->hd', cached_weights, value_heads) + own_weights[:, None] * new_value.astype(jnp.float32).reshape(HEADS, HEAD_DIM)
        return mixed.astype(jnp.bfloat16).reshape(HEADS * HEAD_DIM)
    dec_attention = lax.map(one_sequence, (dec_queries, dec_new_keys, dec_new_values, dec_gate_now, dec_keys, dec_values, dec_gates, dec_lengths))
    piece_out = jnp.dot(piece_attention, out_weight, preferred_element_type=jnp.float32).astype(jnp.bfloat16)
    dec_out = jnp.dot(dec_attention, out_weight, preferred_element_type=jnp.float32).astype(jnp.bfloat16)
    return (piece_out, dec_out, piece_keys, piece_values)
```

```python
import functools
import math

import jax
import jax.numpy as jnp
from jax import lax
from jax.experimental import pallas as pl
from jax.experimental.pallas import tpu as pltpu
from jax.sharding import PartitionSpec as P

norm_eps = 1e-05
LOG2E = math.log2(math.e)
MESH = pl.DeviceIdType.MESH
NT = (((1,), (1,)), ((), ()))
F32 = jnp.float32
BF16 = jnp.bfloat16


def xor(a, k, n):
    out, bit = 0, 1
    while bit < n:
        out = out + ((a // bit + k // bit) % 2) * bit
        bit *= 2
    return out


def rms(values, gain):
    factor = lax.rsqrt(jnp.mean(values * values, axis=-1, keepdims=True) + norm_eps)
    return values * factor * gain


def lane_fold(op, values):
    out = values[:, :128]
    for i in range(1, values.shape[1] // 128):
        out = op(out, values[:, i * 128 : (i + 1) * 128])
    return out


def kernel(
    n, t, heads,
    piece_x, dec_x, gain, qw, kw, vw, fwt, fb, ow, ck, cv, cg, dk, dv, dg, dl,
    out_p, out_d, out_k, out_v,
    xs, qws, kws, vws, ows, cks, cvs, dks, dvs,
    normed, qall, tots, numsend, numrecv, statsend, statrecv, attn_own, attn_recv,
    kbuf, vbuf, cgs, dgs, pbias, sbuf,
    load_sem, store_sem, q_ssem, q_rsem, t_ssem, t_rsem, n_ssem, n_rsem, s_ssem, s_rsem, a_ssem, a_rsem,
):
    me = lax.axis_index("kv")
    tp = lax.axis_index("tp")
    rows = xs.shape[0]
    all_rows = normed.shape[0]
    width = qws.shape[1]
    hd = width // heads
    dec = dec_x.shape[0]
    cache_rows = cks.shape[0]
    span = dks.shape[1]
    scale = hd ** (-0.5)
    scale2 = scale * LOG2E

    loads = [
        pltpu.make_async_copy(src, dst, load_sem.at[i])
        for i, (src, dst) in enumerate(
            [(piece_x, xs), (qw, qws), (kw, kws), (vw, vws), (dk, dks), (dv, dvs), (ck, cks), (cv, cvs), (ow, ows)]
        )
    ]
    for i in range(4):
        loads[i].start()

    barrier = pltpu.get_barrier_semaphore()
    for k in range(1, n):
        pl.semaphore_signal(barrier, inc=1, device_id={"kv": xor(me, k, n)}, device_id_type=MESH)
    for k in range(1, t):
        pl.semaphore_signal(barrier, inc=1, device_id={"tp": lax.rem(tp + k, t)}, device_id_type=MESH)

    g = gain[...]
    dec_normed = rms(dec_x[...].astype(F32), g)
    pad = all_rows - rows - dec
    normed[rows:, :] = jnp.concatenate([dec_normed, jnp.zeros((pad, g.shape[1]), F32)], 0).astype(BF16)
    loads[0].wait()
    step = 64
    for i in range(0, rows, step):
        normed[i : i + step, :] = rms(xs[i : i + step, :].astype(F32), g).astype(BF16)
    for i in range(4, 9):
        loads[i].start()
    loads[1].wait()
    q = jnp.dot(normed[...], qws[...], preferred_element_type=F32).astype(BF16)
    qall[0] = q[:rows]
    dec_q = q[rows:].astype(F32)
    pl.semaphore_wait(barrier, n - 1 + t - 1)

    def q_copy(k):
        return pltpu.make_async_remote_copy(
            src_ref=qall.at[0], dst_ref=qall.at[k], send_sem=q_ssem.at[k], recv_sem=q_rsem.at[k],
            device_id={"kv": xor(me, k, n)}, device_id_type=MESH)

    def t_copy(k):
        return pltpu.make_async_remote_copy(
            src_ref=tots.at[0], dst_ref=tots.at[k], send_sem=t_ssem.at[k], recv_sem=t_rsem.at[k],
            device_id={"kv": xor(me, k, n)}, device_id_type=MESH)

    def n_copy(k):
        return pltpu.make_async_remote_copy(
            src_ref=numsend.at[k], dst_ref=numrecv.at[k], send_sem=n_ssem.at[k], recv_sem=n_rsem.at[k],
            device_id={"kv": xor(me, k, n)}, device_id_type=MESH)

    def s_copy(k):
        return pltpu.make_async_remote_copy(
            src_ref=statsend.at[k], dst_ref=statrecv.at[k], send_sem=s_ssem.at[k], recv_sem=s_rsem.at[k],
            device_id={"kv": xor(me, k, n)}, device_id_type=MESH)

    for k in range(1, n):
        q_copy(k).start()

    z = lax.dot_general(fwt[...], normed[...], NT, preferred_element_type=F32) + fb[...]
    log_gates = jnp.minimum(z, 0.0) - jnp.log1p(jnp.exp(-jnp.abs(z)))
    earlier = lax.broadcasted_iota(jnp.int32, (rows, rows), 0) <= lax.broadcasted_iota(jnp.int32, (rows, rows), 1)
    running = lax.dot_general(
        log_gates[:, :rows], earlier.astype(F32), (((1,), (0,)), ((), ())),
        precision=lax.Precision.HIGHEST, preferred_element_type=F32)
    tots[0] = jnp.zeros((8, 128), F32)
    tots[0, :heads, :] = jnp.broadcast_to(running[:, rows - 1 :], (heads, 128))
    for k in range(1, n):
        t_copy(k).start()

    loads[2].wait()
    keys = jnp.dot(normed[...], kws[...], preferred_element_type=F32).astype(BF16)
    kbuf[...] = keys[:rows]
    dec_k = keys[rows:].astype(F32)
    loads[3].wait()
    values = jnp.dot(normed[...], vws[...], preferred_element_type=F32).astype(BF16)
    vbuf[...] = values[:rows]
    dec_v = values[rows:].astype(F32)
    stores = [pltpu.make_async_copy(kbuf, out_k, store_sem.at[0]), pltpu.make_async_copy(vbuf, out_v, store_sem.at[1])]
    for copy in stores:
        copy.start()

    cgs[...] = cg[...] * LOG2E

    drows = dgs.shape[0]
    row_w = lax.broadcasted_iota(jnp.int32, (drows, width), 0)
    lane_w = lax.broadcasted_iota(jnp.int32, (drows, width), 1)
    masks = [(row_w == b * heads + lane_w // hd) for b in range(dec)]
    row_1 = lax.broadcasted_iota(jnp.int32, (drows, 1), 0)
    if drows > dec * heads:
        dgs[...] = jnp.zeros(dgs.shape, F32)
    own_score = jnp.zeros((drows, 1), F32)
    live = jnp.ones((drows, 1), jnp.int32)
    now = jnp.zeros((drows, 1), F32)
    loads[4].wait()
    scores = jnp.zeros((drows, span), F32)
    for b in range(dec):
        dgs[b * heads : (b + 1) * heads, :] = dg[b]
        qb = jnp.where(masks[b], jnp.broadcast_to(dec_q[b : b + 1], (drows, width)), 0.0)
        own_score = own_score + jnp.sum(qb * dec_k[b : b + 1], axis=1, keepdims=True)
        live = jnp.where(row_1 // heads == b, dl[b], live)
        for h in range(heads):
            now = jnp.where(row_1 == b * heads + h, log_gates[h : h + 1, rows + b : rows + b + 1], now)
        scores = scores + lax.dot_general(qb.astype(BF16), dks[b], NT, preferred_element_type=F32)
    scores = scores * scale2 + (dgs[...] + now) * LOG2E
    scores = jnp.where(lax.broadcasted_iota(jnp.int32, (drows, span), 1) < live, scores, -jnp.inf)
    own_score = own_score * scale2
    top = jnp.maximum(jnp.max(scores, axis=1, keepdims=True), own_score)
    e = jnp.exp2(scores - top)
    own_e = jnp.exp2(own_score - top)
    whole = jnp.sum(e, axis=1, keepdims=True) + own_e
    w = (e / whole).astype(BF16)
    own_w = (own_e / whole).astype(BF16).astype(F32)
    loads[5].wait()
    outs = []
    for b in range(dec):
        mixed = jnp.dot(w, dvs[b], preferred_element_type=F32) + own_w * dec_v[b : b + 1]
        outs.append(jnp.sum(jnp.where(masks[b], mixed, 0.0), axis=0, keepdims=True))
    outs.append(jnp.zeros((pad, width), F32))
    attn_own[rows:, :] = jnp.concatenate(outs, 0).astype(BF16)

    offset = jnp.zeros((8, 128), F32)
    for k in range(1, n):
        t_copy(k).wait_recv()
        offset = offset + jnp.where(xor(me, k, n) < me, tots[k], 0.0)
    pbias[...] = -(running + offset[:heads, :1]) * LOG2E

    loads[6].wait()
    loads[7].wait()
    lane_s = lax.broadcasted_iota(jnp.int32, (rows, 128), 1)
    chunk = math.gcd(cache_rows, 1024)

    def attend(lap, carry):
        k = lax.rem(lap, n)

        @pl.when(k != 0)
        def _():
            q_copy(k).wait_recv()

        owner = xor(me, k, n)
        first = owner * rows - me * rows
        stats = jnp.zeros((rows, 128), F32)
        for h in range(heads):
            hs = slice(h * hd, (h + 1) * hd)
            qh = qall[k, :, hs]
            s = lax.dot_general(qh, kbuf[:, hs], NT, preferred_element_type=F32) * scale2 + pbias[h : h + 1, :]
            seen = lax.broadcasted_iota(jnp.int32, (rows, rows), 1) <= lax.broadcasted_iota(jnp.int32, (rows, rows), 0) + first
            s = jnp.where(seen, s, -jnp.inf)
            sbuf[h, :, cache_rows:] = s
            top = lane_fold(jnp.maximum, s)
            for c in range(0, cache_rows, chunk):
                s = lax.dot_general(qh, cks[c : c + chunk, hs], NT, preferred_element_type=F32) * scale2 + cgs[h : h + 1, c : c + chunk]
                sbuf[h, :, c : c + chunk] = s
                top = jnp.maximum(top, lane_fold(jnp.maximum, s))
            m = jnp.max(top, axis=1, keepdims=True)
            p = jnp.exp2(sbuf[h, :, cache_rows:] - m)
            total = lane_fold(jnp.add, p)
            o = jnp.dot(p.astype(BF16), vbuf[:, hs], preferred_element_type=F32)
            for c in range(0, cache_rows, chunk):
                p = jnp.exp2(sbuf[h, :, c : c + chunk] - m)
                total = total + lane_fold(jnp.add, p)
                o = o + jnp.dot(p.astype(BF16), cvs[c : c + chunk, hs], preferred_element_type=F32)
            l = jnp.sum(total, axis=1, keepdims=True)
            numsend[k, :, hs] = o.astype(BF16)
            stats = jnp.where(lane_s == 2 * h, m, jnp.where(lane_s == 2 * h + 1, l, stats))
        statsend[k] = stats.T[: statsend.shape[1]]

        @pl.when(k != 0)
        def _():
            n_copy(k).start()
            s_copy(k).start()

        return carry

    lax.fori_loop(1, n + 1, attend, 0)

    stats = [statsend[0]]
    for k in range(1, n):
        s_copy(k).wait_recv()
        stats.append(statrecv[k])
    weights = []
    for h in range(heads):
        m = stats[0][2 * h : 2 * h + 1]
        for k in range(1, n):
            m = jnp.maximum(m, stats[k][2 * h : 2 * h + 1])
        fs = [jnp.exp2(s[2 * h : 2 * h + 1] - m) for s in stats]
        l = fs[0] * stats[0][2 * h + 1 : 2 * h + 2]
        for k in range(1, n):
            l = l + fs[k] * stats[k][2 * h + 1 : 2 * h + 2]
        weights += [f / l for f in fs]
    weights.append(jnp.zeros((128 - heads * n, rows), F32))
    cols = jnp.concatenate(weights, 0).T
    for k in range(1, n):
        n_copy(k).wait_recv()
    for h in range(heads):
        hs = slice(h * hd, (h + 1) * hd)
        acc = numsend[0, :, hs].astype(F32) * cols[:, h * n : h * n + 1]
        for k in range(1, n):
            acc = acc + numrecv[k, :, hs].astype(F32) * cols[:, h * n + k : h * n + k + 1]
        attn_own[:rows, hs] = acc.astype(BF16)

    mate = tp + 1 - 2 * (tp % 2)

    def a_copy(k):
        return pltpu.make_async_remote_copy(
            src_ref=attn_own, dst_ref=attn_recv.at[k], send_sem=a_ssem.at[k], recv_sem=a_rsem.at[k],
            device_id={"tp": (tp + k) % t}, device_id_type=MESH)

    def b_copy(k):
        return pltpu.make_async_remote_copy(
            src_ref=attn_recv.at[k], dst_ref=attn_recv.at[k + 1], send_sem=a_ssem.at[k + 1], recv_sem=a_rsem.at[k + 1],
            device_id={"tp": mate}, device_id_type=MESH)

    mate_copy = pltpu.make_async_remote_copy(
        src_ref=attn_own, dst_ref=attn_recv.at[1], send_sem=a_ssem.at[1], recv_sem=a_rsem.at[1],
        device_id={"tp": mate}, device_id_type=MESH)
    for k in range(2, t, 2):
        a_copy(k).start()
    mate_copy.start()
    loads[8].wait()

    def part(block, who):
        return jnp.dot(block, ows[pl.ds(pl.multiple_of(who * width, width), width), :], preferred_element_type=F32)

    acc = part(attn_own[...], tp)
    mate_copy.wait_recv()
    acc = acc + part(attn_recv[1], mate)
    for k in range(2, t, 2):
        a_copy(k).wait_recv()
        b_copy(k).start()
        acc = acc + part(attn_recv[k], (tp + t - k) % t)
    for k in range(2, t, 2):
        b_copy(k).wait_recv()
        acc = acc + part(attn_recv[k + 1], (mate + t - k) % t)
    out_p[...] = acc[:rows].astype(BF16)
    out_d[...] = acc[rows : rows + dec].astype(BF16)

    for copy in stores:
        copy.wait()
    for k in range(1, n):
        q_copy(k).wait_send()
        t_copy(k).wait_send()
        n_copy(k).wait_send()
        s_copy(k).wait_send()
    mate_copy.wait_send()
    for k in range(2, t, 2):
        a_copy(k).wait_send()
        b_copy(k).wait_send()


def shards(
    n, t,
    piece_tokens, dec_tokens, norm_gain, query_weight, key_weight, value_weight, forget_weight, forget_bias,
    out_weight, cache_keys, cache_values, cache_gates, dec_keys, dec_values, dec_gates, dec_lengths,
):
    rows, depth = piece_tokens.shape
    heads = forget_weight.shape[1]
    width = query_weight.shape[1]
    dec = dec_tokens.shape[0]
    all_rows = rows + -(-dec // 16) * 16
    cols = out_weight.shape[1]
    cache_rows = cache_keys.shape[0]
    drows = -(-dec * heads // 8) * 8
    stat_rows = -(-2 * heads // 8) * 8
    any_space = pl.BlockSpec(memory_space=pl.ANY)
    vmem = pl.BlockSpec(memory_space=pltpu.VMEM)
    smem = pl.BlockSpec(memory_space=pltpu.SMEM)

    def like(array):
        return pltpu.VMEM(array.shape, array.dtype)

    dma = pltpu.SemaphoreType.DMA
    return pl.pallas_call(
        functools.partial(kernel, n, t, heads),
        out_shape=(
            jax.ShapeDtypeStruct((rows, cols), BF16),
            jax.ShapeDtypeStruct((dec, cols), BF16),
            jax.ShapeDtypeStruct((rows, width), BF16),
            jax.ShapeDtypeStruct((rows, width), BF16),
        ),
        in_specs=[any_space, vmem, vmem, any_space, any_space, any_space, vmem, vmem, any_space,
                  any_space, any_space, vmem, any_space, any_space, vmem, smem],
        out_specs=(vmem, vmem, any_space, any_space),
        scratch_shapes=[
            like(piece_tokens), like(query_weight), like(key_weight), like(value_weight), like(out_weight),
            like(cache_keys), like(cache_values), like(dec_keys), like(dec_values),
            pltpu.VMEM((all_rows, depth), BF16),
            pltpu.VMEM((n, rows, width), BF16),
            pltpu.VMEM((n, 8, 128), F32),
            pltpu.VMEM((n, rows, width), BF16),
            pltpu.VMEM((n, rows, width), BF16),
            pltpu.VMEM((n, stat_rows, rows), F32),
            pltpu.VMEM((n, stat_rows, rows), F32),
            pltpu.VMEM((all_rows, width), BF16),
            pltpu.VMEM((t, all_rows, width), BF16),
            pltpu.VMEM((rows, width), BF16),
            pltpu.VMEM((rows, width), BF16),
            like(cache_gates),
            pltpu.VMEM((drows, dec_keys.shape[1]), F32),
            pltpu.VMEM((heads, rows), F32),
            pltpu.VMEM((heads, rows, cache_rows + rows), F32),
            dma((9,)), dma((2,)),
            dma((n,)), dma((n,)), dma((n,)), dma((n,)), dma((n,)), dma((n,)), dma((n,)), dma((n,)),
            dma((t,)), dma((t,)),
        ],
        compiler_params=pltpu.CompilerParams(
            collective_id=0, has_side_effects=True, vmem_limit_bytes=60 * 1024 * 1024),
    )(
        piece_tokens, dec_tokens, norm_gain.reshape(1, depth), query_weight, key_weight, value_weight,
        forget_weight.T, forget_bias.reshape(heads, 1), out_weight, cache_keys, cache_values, cache_gates,
        dec_keys, dec_values, dec_gates, dec_lengths,
    )


def solution(mesh):
    rows = P(("grp", "kv"), None)
    both = P(("grp", "kv"), "tp")
    cols = P(None, "tp")
    deep = P(("grp", "kv"), None, "tp")
    return jax.shard_map(
        functools.partial(shards, mesh.shape["kv"], mesh.shape["tp"]),
        mesh=mesh,
        in_specs=(
            rows, rows, P(), cols, cols, cols, cols, P("tp"), cols, both, both, P("tp", ("grp", "kv")),
            deep, deep, P(("grp", "kv"), "tp", None), P(("grp", "kv")),
        ),
        out_specs=(both, both, both, both),
        check_vma=False,
    )
```

```python
import functools
import math

import jax
import jax.numpy as jnp
from jax import lax
from jax.experimental import pallas as pl
from jax.experimental.pallas import tpu as pltpu
from jax.sharding import PartitionSpec as P

norm_eps = 1e-05
LOG2E = math.log2(math.e)
MESH = pl.DeviceIdType.MESH
NT = (((1,), (1,)), ((), ()))
F32 = jnp.float32
BF16 = jnp.bfloat16


def xor(a, k, n):
    out, bit = 0, 1
    while bit < n:
        out = out + ((a // bit + k // bit) % 2) * bit
        bit *= 2
    return out


def rms(values, gain):
    factor = lax.rsqrt(jnp.mean(values * values, axis=-1, keepdims=True) + norm_eps)
    return values * factor * gain


def lane_fold(op, values):
    out = values[:, :128]
    for i in range(1, values.shape[1] // 128):
        out = op(out, values[:, i * 128 : (i + 1) * 128])
    return out


def kernel(
    n, t, heads,
    piece_x, dec_x, gain, qw, kw, vw, fwt, fb, ow, ck, cv, cg, dk, dv, dg, dl,
    out_p, out_d, out_k, out_v,
    xs, qws, kws, vws, ows, cks, cvs, dks, dvs,
    normed, qall, tots, numsend, numrecv, statsend, statrecv, attn_own, attn_recv,
    kbuf, vbuf, cgs, dgs, pbias, sbuf,
    load_sem, store_sem, q_ssem, q_rsem, t_ssem, t_rsem, n_ssem, n_rsem, s_ssem, s_rsem, a_ssem, a_rsem,
):
    me = lax.axis_index("kv")
    tp = lax.axis_index("tp")
    rows = xs.shape[0]
    all_rows = normed.shape[0]
    width = qws.shape[1]
    hd = width // heads
    dec = dec_x.shape[0]
    cache_rows = cks.shape[0]
    span = dks.shape[1]
    scale = hd ** (-0.5)
    scale2 = scale * LOG2E

    loads = [
        pltpu.make_async_copy(src, dst, load_sem.at[i])
        for i, (src, dst) in enumerate(
            [(piece_x, xs), (qw, qws), (kw, kws), (vw, vws), (dk, dks), (dv, dvs), (ck, cks), (cv, cvs), (ow, ows)]
        )
    ]
    for i in range(4):
        loads[i].start()

    barrier = pltpu.get_barrier_semaphore()
    for k in range(1, n):
        pl.semaphore_signal(barrier, inc=1, device_id={"kv": xor(me, k, n)}, device_id_type=MESH)
    for k in range(1, t):
        pl.semaphore_signal(barrier, inc=1, device_id={"tp": lax.rem(tp + k, t)}, device_id_type=MESH)

    g = gain[...]
    dec_normed = rms(dec_x[...].astype(F32), g)
    pad = all_rows - rows - dec
    normed[rows:, :] = jnp.concatenate([dec_normed, jnp.zeros((pad, g.shape[1]), F32)], 0).astype(BF16)
    loads[0].wait()
    step = 64
    for i in range(0, rows, step):
        normed[i : i + step, :] = rms(xs[i : i + step, :].astype(F32), g).astype(BF16)
    for i in range(4, 9):
        loads[i].start()
    loads[1].wait()
    q = jnp.dot(normed[...], qws[...], preferred_element_type=F32).astype(BF16)
    qall[0] = q[:rows]
    dec_q = q[rows:].astype(F32)
    pl.semaphore_wait(barrier, n - 1 + t - 1)

    def q_copy(k):
        return pltpu.make_async_remote_copy(
            src_ref=qall.at[0], dst_ref=qall.at[k], send_sem=q_ssem.at[k], recv_sem=q_rsem.at[k],
            device_id={"kv": xor(me, k, n)}, device_id_type=MESH)

    def t_copy(k):
        return pltpu.make_async_remote_copy(
            src_ref=tots.at[0], dst_ref=tots.at[k], send_sem=t_ssem.at[k], recv_sem=t_rsem.at[k],
            device_id={"kv": xor(me, k, n)}, device_id_type=MESH)

    def n_copy(k, h):
        return pltpu.make_async_remote_copy(
            src_ref=numsend.at[k, h], dst_ref=numrecv.at[k, h], send_sem=n_ssem.at[k, h], recv_sem=n_rsem.at[k, h],
            device_id={"kv": xor(me, k, n)}, device_id_type=MESH)

    def s_copy(k):
        return pltpu.make_async_remote_copy(
            src_ref=statsend.at[k], dst_ref=statrecv.at[k], send_sem=s_ssem.at[k], recv_sem=s_rsem.at[k],
            device_id={"kv": xor(me, k, n)}, device_id_type=MESH)

    for k in range(n - 1, 0, -1):
        q_copy(k).start()

    z = lax.dot_general(fwt[...], normed[...], NT, preferred_element_type=F32)
    bias = jnp.zeros(z.shape, F32)
    for h in range(heads):
        bias = jnp.where(lax.broadcasted_iota(jnp.int32, z.shape, 0) == h, fb[h], bias)
    z = z + bias
    log_gates = jnp.minimum(z, 0.0) - jnp.log1p(jnp.exp(-jnp.abs(z)))
    earlier = lax.broadcasted_iota(jnp.int32, (rows, rows), 0) <= lax.broadcasted_iota(jnp.int32, (rows, rows), 1)
    running = lax.dot_general(
        log_gates[:, :rows], earlier.astype(F32), (((1,), (0,)), ((), ())),
        precision=lax.Precision.HIGHEST, preferred_element_type=F32)
    tots[0] = jnp.zeros((8, 128), F32)
    tots[0, :heads, :] = jnp.broadcast_to(running[:, rows - 1 :], (heads, 128))
    for k in range(1, n):
        t_copy(k).start()

    loads[2].wait()
    keys = jnp.dot(normed[...], kws[...], preferred_element_type=F32).astype(BF16)
    kbuf[...] = keys[:rows]
    dec_k = keys[rows:].astype(F32)
    loads[3].wait()
    values = jnp.dot(normed[...], vws[...], preferred_element_type=F32).astype(BF16)
    vbuf[...] = values[:rows]
    dec_v = values[rows:].astype(F32)
    stores = [pltpu.make_async_copy(kbuf, out_k, store_sem.at[0]), pltpu.make_async_copy(vbuf, out_v, store_sem.at[1])]
    for copy in stores:
        copy.start()

    cgs[...] = cg[...] * LOG2E

    drows = dgs.shape[0]
    row_w = lax.broadcasted_iota(jnp.int32, (drows, width), 0)
    lane_w = lax.broadcasted_iota(jnp.int32, (drows, width), 1)
    masks = [(row_w == b * heads + lane_w // hd) for b in range(dec)]
    row_1 = lax.broadcasted_iota(jnp.int32, (drows, 1), 0)
    if drows > dec * heads:
        dgs[...] = jnp.zeros(dgs.shape, F32)
    own_score = jnp.zeros((drows, 1), F32)
    live = jnp.ones((drows, 1), jnp.int32)
    now = jnp.zeros((drows, 1), F32)
    loads[4].wait()
    scores = jnp.zeros((drows, span), F32)
    for b in range(dec):
        dgs[b * heads : (b + 1) * heads, :] = dg[b]
        qb = jnp.where(masks[b], jnp.broadcast_to(dec_q[b : b + 1], (drows, width)), 0.0)
        own_score = own_score + jnp.sum(qb * dec_k[b : b + 1], axis=1, keepdims=True)
        live = jnp.where(row_1 // heads == b, dl[b], live)
        for h in range(heads):
            now = jnp.where(row_1 == b * heads + h, log_gates[h : h + 1, rows + b : rows + b + 1], now)
        scores = scores + lax.dot_general(qb.astype(BF16), dks[b], NT, preferred_element_type=F32)
    scores = scores * scale2 + (dgs[...] + now) * LOG2E
    scores = jnp.where(lax.broadcasted_iota(jnp.int32, (drows, span), 1) < live, scores, -jnp.inf)
    own_score = own_score * scale2
    top = jnp.maximum(jnp.max(scores, axis=1, keepdims=True), own_score)
    e = jnp.exp2(scores - top)
    own_e = jnp.exp2(own_score - top)
    whole = jnp.sum(e, axis=1, keepdims=True) + own_e
    w = (e / whole).astype(BF16)
    own_w = (own_e / whole).astype(BF16).astype(F32)
    loads[5].wait()
    outs = []
    for b in range(dec):
        mixed = jnp.dot(w, dvs[b], preferred_element_type=F32) + own_w * dec_v[b : b + 1]
        outs.append(jnp.sum(jnp.where(masks[b], mixed, 0.0), axis=0, keepdims=True))
    outs.append(jnp.zeros((pad, width), F32))
    dec_attn = jnp.concatenate(outs, 0).astype(BF16)
    for h in range(heads):
        attn_own[h, rows:, :] = dec_attn[:, h * hd : (h + 1) * hd]

    offset = jnp.zeros((8, 128), F32)
    for k in range(1, n):
        t_copy(k).wait_recv()
        offset = offset + jnp.where(xor(me, k, n) < me, tots[k], 0.0)
    pbias[...] = -(running + offset[:heads, :1]) * LOG2E

    loads[6].wait()
    loads[7].wait()
    lane_s = lax.broadcasted_iota(jnp.int32, (rows, 128), 1)
    chunk = math.gcd(cache_rows, 1024)

    def attend(lap, carry):
        k = lax.rem(2 * n - lap, n)

        @pl.when(k != 0)
        def _():
            q_copy(k).wait_recv()

        owner = xor(me, k, n)
        first = owner * rows - me * rows
        stats = jnp.zeros((rows, 128), F32)
        for h in range(heads):
            hs = slice(h * hd, (h + 1) * hd)
            qh = qall[k, :, hs]
            s = lax.dot_general(qh, kbuf[:, hs], NT, preferred_element_type=F32) * scale2 + pbias[h : h + 1, :]
            seen = lax.broadcasted_iota(jnp.int32, (rows, rows), 1) <= lax.broadcasted_iota(jnp.int32, (rows, rows), 0) + first
            s = jnp.where(seen, s, -jnp.inf)
            sbuf[h, :, cache_rows:] = s
            top = lane_fold(jnp.maximum, s)
            for c in range(0, cache_rows, chunk):
                s = lax.dot_general(qh, cks[c : c + chunk, hs], NT, preferred_element_type=F32) * scale2 + cgs[h : h + 1, c : c + chunk]
                sbuf[h, :, c : c + chunk] = s
                top = jnp.maximum(top, lane_fold(jnp.maximum, s))
            m = jnp.max(top, axis=1, keepdims=True)
            p = jnp.exp2(sbuf[h, :, cache_rows:] - m)
            total = lane_fold(jnp.add, p)
            o = jnp.dot(p.astype(BF16), vbuf[:, hs], preferred_element_type=F32)
            for c in range(0, cache_rows, chunk):
                p = jnp.exp2(sbuf[h, :, c : c + chunk] - m)
                total = total + lane_fold(jnp.add, p)
                o = o + jnp.dot(p.astype(BF16), cvs[c : c + chunk, hs], preferred_element_type=F32)
            l = jnp.sum(total, axis=1, keepdims=True)
            numsend[k, h] = o.astype(BF16)

            @pl.when(k != 0)
            def _():
                n_copy(k, h).start()

            stats = jnp.where(lane_s == 2 * h, m, jnp.where(lane_s == 2 * h + 1, l, stats))
        statsend[k] = stats.T[: statsend.shape[1]]

        @pl.when(k != 0)
        def _():
            s_copy(k).start()

        return carry

    lax.fori_loop(1, n + 1, attend, 0)

    mate = tp + 1 - 2 * (tp % 2)

    def a_copy(k, h):
        return pltpu.make_async_remote_copy(
            src_ref=attn_own.at[h], dst_ref=attn_recv.at[k, h], send_sem=a_ssem.at[k, h], recv_sem=a_rsem.at[k, h],
            device_id={"tp": (tp + k) % t}, device_id_type=MESH)

    def b_copy(k, h):
        return pltpu.make_async_remote_copy(
            src_ref=attn_recv.at[k, h], dst_ref=attn_recv.at[k + 1, h], send_sem=a_ssem.at[k + 1, h], recv_sem=a_rsem.at[k + 1, h],
            device_id={"tp": mate}, device_id_type=MESH)

    def mate_copy(h):
        return pltpu.make_async_remote_copy(
            src_ref=attn_own.at[h], dst_ref=attn_recv.at[1, h], send_sem=a_ssem.at[1, h], recv_sem=a_rsem.at[1, h],
            device_id={"tp": mate}, device_id_type=MESH)

    stats = [statsend[0]]
    for k in range(1, n):
        s_copy(k).wait_recv()
        stats.append(statrecv[k])
    weights = []
    for h in range(heads):
        m = stats[0][2 * h : 2 * h + 1]
        for k in range(1, n):
            m = jnp.maximum(m, stats[k][2 * h : 2 * h + 1])
        fs = [jnp.exp2(s[2 * h : 2 * h + 1] - m) for s in stats]
        l = fs[0] * stats[0][2 * h + 1 : 2 * h + 2]
        for k in range(1, n):
            l = l + fs[k] * stats[k][2 * h + 1 : 2 * h + 2]
        weights += [f / l for f in fs]
    weights.append(jnp.zeros((128 - heads * n, rows), F32))
    cols = jnp.concatenate(weights, 0).T
    for h in range(heads):
        for k in range(1, n):
            n_copy(k, h).wait_recv()
        acc = numsend[0, h].astype(F32) * cols[:, h * n : h * n + 1]
        for k in range(1, n):
            acc = acc + numrecv[k, h].astype(F32) * cols[:, h * n + k : h * n + k + 1]
        attn_own[h, :rows, :] = acc.astype(BF16)
        for k in range(2, t, 2):
            a_copy(k, h).start()
        mate_copy(h).start()

    loads[8].wait()

    def part(block, who):
        block = jnp.concatenate([block[h] for h in range(heads)], 1)
        return jnp.dot(block, ows[pl.ds(pl.multiple_of(who * width, width), width), :], preferred_element_type=F32)

    acc = part(attn_own[...], tp)
    for h in range(heads):
        mate_copy(h).wait_recv()
    acc = acc + part(attn_recv[1], mate)
    for k in range(2, t, 2):
        for h in range(heads):
            a_copy(k, h).wait_recv()
            b_copy(k, h).start()
        acc = acc + part(attn_recv[k], (tp + t - k) % t)
    for k in range(2, t, 2):
        for h in range(heads):
            b_copy(k, h).wait_recv()
        acc = acc + part(attn_recv[k + 1], (mate + t - k) % t)
    out_p[...] = acc[:rows].astype(BF16)
    out_d[...] = acc[rows : rows + dec].astype(BF16)

    for copy in stores:
        copy.wait()
    for k in range(1, n):
        q_copy(k).wait_send()
        t_copy(k).wait_send()
        for h in range(heads):
            n_copy(k, h).wait_send()
        s_copy(k).wait_send()
    for h in range(heads):
        mate_copy(h).wait_send()
        for k in range(2, t, 2):
            a_copy(k, h).wait_send()
            b_copy(k, h).wait_send()


def hand_over(*refs):
    for src, dst in zip(refs[:4], refs[4:]):
        dst[...] = src[...]


def shards(
    n, t,
    piece_tokens, dec_tokens, norm_gain, query_weight, key_weight, value_weight, forget_weight, forget_bias,
    out_weight, cache_keys, cache_values, cache_gates, dec_keys, dec_values, dec_gates, dec_lengths,
):
    rows, depth = piece_tokens.shape
    heads = forget_weight.shape[1]
    width = query_weight.shape[1]
    dec = dec_tokens.shape[0]
    all_rows = rows + -(-dec // 16) * 16
    cols = out_weight.shape[1]
    cache_rows = cache_keys.shape[0]
    drows = -(-dec * heads // 8) * 8
    stat_rows = -(-2 * heads // 8) * 8
    any_space = pl.BlockSpec(memory_space=pl.ANY)
    vmem = pl.BlockSpec(memory_space=pltpu.VMEM)
    smem = pl.BlockSpec(memory_space=pltpu.SMEM)

    def like(array):
        return pltpu.VMEM(array.shape, array.dtype)

    dma = pltpu.SemaphoreType.DMA
    parts = pl.pallas_call(
        functools.partial(kernel, n, t, heads),
        out_shape=(
            jax.ShapeDtypeStruct((rows, cols), BF16),
            jax.ShapeDtypeStruct((dec, cols), BF16),
            jax.ShapeDtypeStruct((rows, width), BF16),
            jax.ShapeDtypeStruct((rows, width), BF16),
        ),
        in_specs=[any_space, vmem, vmem, any_space, any_space, any_space, vmem, smem, any_space,
                  any_space, any_space, vmem, any_space, any_space, vmem, smem],
        out_specs=(vmem, vmem, any_space, any_space),
        scratch_shapes=[
            like(piece_tokens), like(query_weight), like(key_weight), like(value_weight), like(out_weight),
            like(cache_keys), like(cache_values), like(dec_keys), like(dec_values),
            pltpu.VMEM((all_rows, depth), BF16),
            pltpu.VMEM((n, rows, width), BF16),
            pltpu.VMEM((n, 8, 128), F32),
            pltpu.VMEM((n, heads, rows, width // heads), BF16),
            pltpu.VMEM((n, heads, rows, width // heads), BF16),
            pltpu.VMEM((n, stat_rows, rows), F32),
            pltpu.VMEM((n, stat_rows, rows), F32),
            pltpu.VMEM((heads, all_rows, width // heads), BF16),
            pltpu.VMEM((t, heads, all_rows, width // heads), BF16),
            pltpu.VMEM((rows, width), BF16),
            pltpu.VMEM((rows, width), BF16),
            like(cache_gates),
            pltpu.VMEM((drows, dec_keys.shape[1]), F32),
            pltpu.VMEM((heads, rows), F32),
            pltpu.VMEM((heads, rows, cache_rows + rows), F32),
            dma((9,)), dma((2,)),
            dma((n,)), dma((n,)), dma((n,)), dma((n,)), dma((n, heads)), dma((n, heads)), dma((n,)), dma((n,)),
            dma((t, heads)), dma((t, heads)),
        ],
        compiler_params=pltpu.CompilerParams(
            collective_id=0, has_side_effects=True, vmem_limit_bytes=60 * 1024 * 1024),
    )(
        piece_tokens, dec_tokens, norm_gain.reshape(1, depth), query_weight, key_weight, value_weight,
        forget_weight.T, forget_bias, out_weight, cache_keys, cache_values, cache_gates,
        dec_keys, dec_values, dec_gates, dec_lengths,
    )
    return pl.pallas_call(
        hand_over,
        out_shape=tuple(jax.ShapeDtypeStruct(p.shape, p.dtype) for p in parts),
        in_specs=[vmem] * 4,
        out_specs=(vmem,) * 4,
    )(*parts)


def solution(mesh):
    rows = P(("grp", "kv"), None)
    both = P(("grp", "kv"), "tp")
    cols = P(None, "tp")
    deep = P(("grp", "kv"), None, "tp")
    return jax.shard_map(
        functools.partial(shards, mesh.shape["kv"], mesh.shape["tp"]),
        mesh=mesh,
        in_specs=(
            rows, rows, P(), cols, cols, cols, cols, P("tp"), cols, both, both, P("tp", ("grp", "kv")),
            deep, deep, P(("grp", "kv"), "tp", None), P(("grp", "kv")),
        ),
        out_specs=(both, both, both, both),
        check_vma=False,
    )
```
